32 devices in a mesh: sp: 16 (over z, y, x), tp: 2 (over core).
Axes of the slice: x: 2, y: 2, z: 4, core: 2. Of those that a mesh axis runs over, the one named last changes fastest.
Arguments:
- tokens: bfloat16 [4096, 3072], P('sp', 'tp'), may hold values from -6 to 6
- norm_gain: float32 [3072], replicated, may hold values from 0.1 to 1.9
- outer_gate_w: bfloat16 [3072, 1536], P('sp', 'tp'), may hold values from -0.109375 to 0.109375
- inner_gate_w: bfloat16 [3072, 1536], P('sp', 'tp'), may hold values from -0.109375 to 0.109375
- signal_w: bfloat16 [3072, 1536], P('sp', 'tp'), may hold values from -0.109375 to 0.109375
- conv_taps: float32 [3, 1536], P(None, 'tp'), may hold values from -3.5 to 3.5
- query_w: bfloat16 [3072, 1536], P('sp', 'tp'), may hold values from -1.5 to 1.5
- key_w: bfloat16 [3072, 512], P('sp', 'tp'), may hold values from -1.5 to 1.5
- value_w: bfloat16 [3072, 512], P('sp', 'tp'), may hold values from -0.109375 to 0.109375
- sink_logits: float32 [24], P('tp'), may hold values from -1 to 5
- out_conv_w: bfloat16 [1536, 3072], P('tp', 'sp'), may hold values from -0.109375 to 0.109375
- out_attn_w: bfloat16 [1536, 3072], P('tp', 'sp'), may hold values from -0.109375 to 0.109375
Outputs:
- mixed: bfloat16 [4096, 3072], P(('sp', 'tp'))
The draws below stay inside these ranges and needn't reach their ends.
All inputs are finite; a program needn't handle non-finite values.
Results may differ from the reference program's by a relative error of at most 0.02.
Values may be sent and summed in bfloat16 or wider, within the bound.
No kernel may reach another device: no remote copies, remote signals or barrier semaphores. Data moves between devices by JAX's collectives and lax.ppermute only.
A program may use at most 64 MiB of HBM per device.

```python
import jax
import jax.numpy as jnp
from jax import lax

D = 3072
CONV = 1536
QHEADS = 24
KVHEADS = 8
HEAD = 64
TAPS = 3
WINDOW = 128
TOKENS = 4096
N_TP = 2


def draw_query_w(key, part):
    drawn = jax.random.normal(jax.random.fold_in(key, 21), (D, QHEADS * HEAD), jnp.float32) * D ** (-0.5)
    return jnp.clip(drawn, -1.5, 1.5).astype(jnp.bfloat16)


def draw_key_w(key, part):
    drawn = jax.random.normal(jax.random.fold_in(key, 22), (D, KVHEADS * HEAD), jnp.float32) * D ** (-0.5)
    return jnp.clip(drawn, -1.5, 1.5).astype(jnp.bfloat16)


def levels(key, dims, split, smallest, largest):
    def one(dim, parts):
        heights = jax.random.uniform(jax.random.fold_in(jax.random.fold_in(key, 6), dim), (parts,), jnp.float32, smallest / len(split), largest / len(split))
        return jnp.repeat(jnp.exp(heights), dims[dim] // parts).reshape((-1,) + (1,) * (len(dims) - dim - 1))

    level = one(*split[0])
    for cut in split[1:]:
        level = level * one(*cut)
    return level


def noise(key, shape, width, most, split=(), kind=jnp.bfloat16):
    entries = jax.random.normal(key, shape, jnp.float32) * width
    if len(split) > 0:
        entries = levels(key, shape, split, -0.22, 0.18) * entries
    return jnp.clip(entries, min=-most, max=most).astype(kind)


def setup_inputs(seed: int = 0) -> dict:
    key_of = jax.random.split(jax.random.key(seed), 13)
    tokens = noise(key_of[0], (TOKENS, D), 1.0, 6.0, ((0, 16), (1, 2)))
    norm_gain = jnp.clip(1.0 + 0.18 * jax.random.normal(key_of[1], (D,), jnp.float32), 0.1, 1.9)
    outer_gate_w = noise(key_of[2], (D, CONV), D ** -0.5, 0.109375, ((0, 16), (1, 2)))
    inner_gate_w = noise(key_of[3], (D, CONV), D ** -0.5, 0.109375, ((0, 16), (1, 2)))
    signal_w = noise(key_of[4], (D, CONV), D ** -0.5, 0.109375, ((0, 16), (1, 2)))
    conv_taps = noise(key_of[5], (TAPS, CONV), TAPS ** -0.5, 3.5, ((1, 2),), jnp.float32)
    query_w = draw_query_w(jax.random.fold_in(key_of[12], 71), 0)
    key_w = draw_key_w(jax.random.fold_in(key_of[12], 71), 0)
    value_w = noise(key_of[8], (D, KVHEADS * HEAD), D ** -0.5, 0.109375, ((0, 16), (1, 2)))
    sink_logits = jnp.clip(-1.0 + 6.0 * jax.random.uniform(key_of[9], (QHEADS,), jnp.float32) ** levels(key_of[9], (QHEADS,), ((0, 2),), -0.2, 0.2), -1.0, 5.0)
    out_conv_w = noise(key_of[10], (CONV, D), (CONV + QHEADS * HEAD) ** -0.5, 0.109375, ((0, 2), (1, 16)))
    out_attn_w = noise(key_of[11], (QHEADS * HEAD, D), (CONV + QHEADS * HEAD) ** -0.5, 0.109375, ((0, 2), (1, 16)))
    return dict(tokens=tokens, norm_gain=norm_gain, outer_gate_w=outer_gate_w, inner_gate_w=inner_gate_w, signal_w=signal_w, conv_taps=conv_taps, query_w=query_w, key_w=key_w, value_w=value_w, sink_logits=sink_logits, out_conv_w=out_conv_w, out_attn_w=out_attn_w)


def reference(tokens, norm_gain, outer_gate_w, inner_gate_w, signal_w, conv_taps, query_w, key_w, value_w, sink_logits, out_conv_w, out_attn_w):
    f32 = jnp.float32
    bf16 = jnp.bfloat16
    x32 = tokens.astype(f32)
    normed = (x32 * lax.rsqrt(lax.optimization_barrier(jnp.mean(x32 * x32, axis=-1, keepdims=True)) + 1e-06) * norm_gain).astype(bf16)

    def project(weight):
        return jnp.dot(normed, weight, preferred_element_type=f32).astype(bf16)
    outer = project(outer_gate_w)
    inner = project(inner_gate_w)
    signal = project(signal_w)
    queries = project(query_w)
    keys = project(key_w)
    values = project(value_w)
    gated = (inner.astype(f32) * signal.astype(f32)).astype(bf16)
    padded = jnp.concatenate([jnp.zeros((TAPS - 1, CONV), bf16), gated], axis=0).astype(f32)
    conv = sum((conv_taps[k] * padded[k:k + TOKENS] for k in range(TAPS)))
    conv_out = (outer.astype(f32) * conv).astype(bf16)
    group = QHEADS // KVHEADS
    span = min(512, TOKENS)
    slopes = jnp.exp2(-8.0 * jnp.arange(1, QHEADS + 1, dtype=f32) / QHEADS).reshape(KVHEADS, group)
    sinks = sink_logits.reshape(KVHEADS, group)[:, :, None]
    keys_pad = jnp.concatenate([jnp.zeros((WINDOW, KVHEADS * HEAD), bf16), keys], axis=0)
    values_pad = jnp.concatenate([jnp.zeros((WINDOW, KVHEADS * HEAD), bf16), values], axis=0)

    def attend(block):
        start = (block * span).astype(jnp.int32)
        qb = lax.dynamic_slice_in_dim(queries, start, span, 0).reshape(span, KVHEADS, group, HEAD).astype(f32)
        kb = lax.dynamic_slice_in_dim(keys_pad, start, span + WINDOW, 0).reshape(span + WINDOW, KVHEADS, HEAD).astype(f32)
        vb = lax.dynamic_slice_in_dim(values_pad, start, span + WINDOW, 0).reshape(span + WINDOW, KVHEADS, HEAD).astype(f32)
        scores = jnp.einsum('qhgd,shd->hgqs', qb, kb) * HEAD ** (-0.5)
        qpos = start + jnp.arange(span, dtype=jnp.int32)
        kpos = start - WINDOW + jnp.arange(span + WINDOW, dtype=jnp.int32)
        dist = qpos[:, None] - kpos[None, :]
        valid = (dist >= 0) & (dist < WINDOW) & (kpos >= 0)[None, :]
        scores = scores - slopes[:, :, None, None] * dist.astype(f32)
        scores = jnp.where(valid, scores, -1e+30)
        top = jnp.maximum(lax.optimization_barrier(jnp.max(scores, axis=-1)), sinks)
        expo = jnp.exp(scores - top[..., None])
        total = lax.optimization_barrier(jnp.sum(expo, axis=-1)) + jnp.exp(sinks - top)
        probs = (expo / total[..., None]).astype(bf16).astype(f32)
        out = jnp.einsum('hgqs,shd->qhgd', probs, vb)
        return out.reshape(span, QHEADS * HEAD)
    attn_out = lax.map(attend, jnp.arange(TOKENS // span, dtype=jnp.int32)).reshape(TOKENS, QHEADS * HEAD).astype(bf16)
    conv_part = CONV // N_TP
    attn_part = QHEADS * HEAD // N_TP
    total_sum = jnp.zeros((TOKENS, D), f32)
    for index in range(N_TP):
        conv_cols = conv_out[:, index * conv_part:(index + 1) * conv_part]
        attn_cols = attn_out[:, index * attn_part:(index + 1) * attn_part]
        partial_value = jnp.dot(conv_cols, out_conv_w[index * conv_part:(index + 1) * conv_part], preferred_element_type=f32)
        partial_value = partial_value + jnp.dot(attn_cols, out_attn_w[index * attn_part:(index + 1) * attn_part], preferred_element_type=f32)
        total_sum = total_sum + partial_value.astype(bf16).astype(f32)
    return total_sum.astype(bf16)
```

```python
import functools

import jax
import jax.numpy as jnp
from jax import lax
from jax.experimental import pallas as pl
from jax.experimental.pallas import tpu as pltpu
from jax.sharding import Mesh
from jax.sharding import PartitionSpec as P

QHEADS = 24
KVHEADS = 8
HEAD = 64
TAPS = 3
WINDOW = 128
EPS = 1e-06
BF16 = jnp.bfloat16
F32 = jnp.float32


PART_FLIP = (0, 2, 1, 3)
VMEM = pl.BlockSpec(memory_space=pltpu.VMEM)
SMEM = pl.BlockSpec(memory_space=pltpu.SMEM)
NT = (((1,), (1,)), ((), ()))


def call(kernel, out_shape, *args, specs, flops, name, grid=(), out_specs=None, scratch=(), limit=40):
    size = sum(a.size * a.dtype.itemsize for a in args)
    outs = out_shape if isinstance(out_shape, (list, tuple)) else [out_shape]
    size += sum(o.size * o.dtype.itemsize for o in outs)
    return pl.pallas_call(
        kernel,
        out_shape=out_shape,
        grid=grid,
        in_specs=specs,
        out_specs=out_specs if out_specs is not None else jax.tree.map(lambda _: VMEM, out_shape),
        scratch_shapes=scratch,
        cost_estimate=pl.CostEstimate(flops=flops, bytes_accessed=size, transcendentals=0),
        compiler_params=pltpu.CompilerParams(vmem_limit_bytes=limit * 1024 * 1024),
        name=name,
    )(*args)


def pack_columns_kernel(count, ids, *refs):
    weights, outs = refs[:count], refs[count:]
    part = ids[1] * 2 + ids[3]
    groups = len(outs)
    for p in range(groups):
        for m in range(groups):

            @pl.when(part == p ^ PART_FLIP[m])
            def _():
                pieces = []
                for w in weights:
                    width = w.shape[1] // groups
                    pieces.append(w[:, p * width : (p + 1) * width])
                outs[m][...] = jnp.concatenate(pieces, axis=1)


def pack_rows_kernel(ids, conv_ref, attn_ref, *outs):
    part = ids[1] * 2 + ids[3]
    groups = len(outs)
    for p in range(groups):
        for m in range(groups):

            @pl.when(part == p ^ PART_FLIP[m])
            def _():
                pieces = []
                for w in (conv_ref, attn_ref):
                    width = w.shape[0] // groups
                    pieces.append(w[p * width : (p + 1) * width, :].astype(F32).T.astype(BF16))
                outs[m][...] = jnp.concatenate(pieces, axis=1)


def norm_kernel(ids, own_ref, other_ref, gain_ref, out_ref):
    t = ids[4]
    blocks, rows, width = out_ref.shape
    here = pl.ds(pl.multiple_of(t * rows, rows), rows)
    own, other = own_ref[here, :].astype(F32), other_ref[here, :].astype(F32)
    total = jnp.sum(own * own, axis=1, keepdims=True) + jnp.sum(other * other, axis=1, keepdims=True)
    scale = lax.rsqrt(total / (blocks * width) + EPS)
    for k in range(blocks):
        side, at = divmod(k, blocks // 2)
        columns = slice(at * width, (at + 1) * width)
        value = jnp.where(t == side, own[:, columns], other[:, columns])
        out_ref[k] = (value * scale * gain_ref[:, k * width : (k + 1) * width]).astype(BF16)


def project_kernel(tail_of, ids, *refs):
    normed, pieces = refs[:8], refs[8:12]
    out_ref, tail_ref, acc = refs[12:]
    s1, g1, s2, g2, t = (ids[i] for i in range(5))
    rows = normed[0].shape[1]
    for a in range(2):
        for b in range(2):
            piece = pieces[a * 2 + b]
            for c in range(2):
                k = (s1 ^ a) * 4 + (g1 ^ c) * 2 + (s2 ^ b)
                right = jnp.concatenate([piece[g2 * 2 + c], piece[(1 - g2) * 2 + c]], axis=0)
                for side in range(2):
                    left = jnp.concatenate([normed[side * 4 + m][k] for m in range(4)], axis=0)
                    value = jnp.dot(left, right, preferred_element_type=F32)
                    span = slice(side * 4 * rows, (side + 1) * 4 * rows)
                    if a + b + c == 0:
                        acc[span, :] = value
                    else:
                        acc[span, :] += value
    for side in range(2):
        for m in range(4):
            at = side * 4 + m
            block = ((g1 * 2 + g2) ^ PART_FLIP[m]) * 2 + (t ^ side)
            out_ref[block] = acc[at * rows : (at + 1) * rows, :].astype(BF16)
    for g in range(2):
        tail_ref[g] = tail_of(out_ref[g * 4 + 3])


def kv_tail(block):
    return jnp.concatenate([block[:, 192:256], block[:, 448:512]], axis=1)


def conv_tail(block):
    return block[-16:, :]


def mixer_kernel(widths, ids, sinks_ref, taps_ref, a_ref, b_ref, kv_along, kv_across, b_along, b_across, out_ref):
    heads, channels = widths
    s1, g1, s2, g2, t = (ids[i] for i in range(5))
    step = pl.program_id(0)
    per_run = pl.num_programs(0) // 2
    run, at = step // per_run, step % per_run
    inside_run = at > 0
    before = jnp.maximum(step - 1, 0)
    q_width = heads * HEAD
    rows = a_ref.shape[1]

    def halo(along, across):
        return jnp.where((s2 == 0) & (run == 0), across[0], along[jnp.where(s2 == 0, 0, run)])

    def split_kv(block):
        return block[:, q_width : q_width + HEAD], block[:, q_width + HEAD + channels :]

    here = a_ref[step]
    keys, values = split_kv(here)
    old_keys, old_values = split_kv(a_ref[before])
    kv = halo(kv_along, kv_across)
    old_keys = jnp.where(inside_run, old_keys, kv[:, :HEAD])
    old_values = jnp.where(inside_run, old_values, kv[:, HEAD:])
    keys = jnp.concatenate([old_keys, keys], axis=0)
    values = jnp.concatenate([old_values, values], axis=0)

    position = lax.broadcasted_iota(jnp.int32, (rows, 2 * rows), 0)
    key_at = lax.broadcasted_iota(jnp.int32, (rows, 2 * rows), 1)
    dist = position + rows - key_at
    first_window = (s1 == 0) & (g1 * 0 + run == 0) & (s2 == 0) & (at == 0)
    valid = (dist >= 0) & (dist < WINDOW) & (key_at >= jnp.where(first_window, rows, 0))
    dist = dist.astype(F32)
    first = ((t * 4 + g1 * 2 + g2) * heads + 1).astype(F32)
    attn = []
    for h in range(heads):
        slope = jnp.exp2(-8.0 * jnp.full((1, 2 * rows), first + h, F32) / QHEADS)
        scores = lax.dot_general(here[:, h * HEAD : (h + 1) * HEAD], keys, NT, preferred_element_type=F32)
        scores = jnp.where(valid, scores * HEAD ** (-0.5) - slope * dist, -1e30)
        sink = jnp.full((rows, 1), sinks_ref[(g1 * 2 + g2) * heads + h], F32)
        top = jnp.maximum(jnp.max(scores, axis=1, keepdims=True), sink)
        expo = jnp.exp(scores - top)
        total = jnp.sum(expo, axis=1, keepdims=True) + jnp.exp(sink - top)
        probs = (expo / total).astype(BF16)
        attn.append(jnp.dot(probs, values, preferred_element_type=F32).astype(BF16))

    def gate(block):
        product = block[:, :channels].astype(F32) * block[:, channels:].astype(F32)
        return product.astype(BF16).astype(F32)

    outer = here[:, q_width + HEAD : q_width + HEAD + channels].astype(F32)
    gated = gate(b_ref[step])
    old = jnp.where(inside_run, b_ref[before][-16:, :], halo(b_along, b_across))
    extended = jnp.concatenate([gate(old), gated], axis=0)
    start = 16 - TAPS + 1
    conv = sum(taps_ref[k : k + 1, :] * extended[start + k : start + k + rows, :] for k in range(TAPS))
    out_ref[0] = jnp.concatenate([(outer * conv).astype(BF16), *attn], axis=1)


def project_out_kernel(count, ids, act_ref, *refs):
    pieces, (sent_ref, kept_ref) = refs[:count], refs[count:]
    s1, g1, s2, g2, t = (ids[i] for i in range(5))
    rows = act_ref.shape[1]
    for out_ref, side in ((sent_ref, 1 - t), (kept_ref, t)):
        left = jnp.concatenate(
            [act_ref[((g1 * 2 + g2) ^ PART_FLIP[m]) * 2 + side] for m in range(4)], axis=0
        )
        for i, piece in enumerate(pieces):
            for g in range(2):
                c = g1 ^ g
                right = jnp.concatenate([piece[g2 * 2 + c], piece[(1 - g2) * 2 + c]], axis=0)
                value = lax.dot_general(left, right, NT, preferred_element_type=F32).astype(BF16)
                width = right.shape[0]
                at = (i * 2 + g) * width
                for m in range(4):
                    out_ref[m, :, at : at + width] = value[m * rows : (m + 1) * rows, :]


def assemble_kernel(order, ids, *refs):
    out_ref = refs[-1]
    s1, s2 = ids[0], ids[2]
    for n, group in enumerate(order):
        kept, got, got2, got3 = refs[n * 4 : n * 4 + 4]
        total = kept[0].astype(F32) + got[0].astype(F32) + got2[0].astype(F32) + got3[...].astype(F32)
        width = total.shape[1] // (2 * len(group))
        for i, (a, b) in enumerate(group):
            for g in range(2):
                at = (((s1 ^ a) * 2 + g) * 2 + (s2 ^ b)) * width
                value = total[:, (i * 2 + g) * width : (i * 2 + g + 1) * width]
                out_ref[:, pl.ds(pl.multiple_of(at, width), width)] = value.astype(BF16)


def swap(value, axis):
    return lax.ppermute(value, axis, [(0, 1), (1, 0)])


def swap_both(value):
    return lax.ppermute(value, ("g1", "g2"), [(i, 3 - i) for i in range(4)])


def struct(*shape, dtype=BF16):
    return jax.ShapeDtypeStruct(shape, dtype)


def body(
    tokens,
    norm_gain,
    outer_gate_w,
    inner_gate_w,
    signal_w,
    conv_taps,
    query_w,
    key_w,
    value_w,
    sink_logits,
    out_conv_w,
    out_attn_w,
):
    ids = jnp.stack([lax.axis_index(a) for a in ("s1", "g1", "s2", "g2", "tp")]).astype(jnp.int32)
    depth = query_w.shape[0]
    rows = tokens.shape[0] // 2
    channels, q_width = outer_gate_w.shape[1] // 4, query_w.shape[1] // 4
    heads = q_width // HEAD
    k_width = 2 * depth
    k_blocks = tokens.shape[1] * 2 // k_width

    other_tokens = swap(tokens, "tp")

    def columns(name, *weights):
        width = sum(w.shape[1] for w in weights) // 4
        return call(
            functools.partial(pack_columns_kernel, len(weights)),
            [struct(depth, width)] * 4,
            ids,
            *weights,
            specs=[SMEM] + [VMEM] * len(weights),
            flops=1 << 20,
            name=name,
        )

    def to_owners(blocks):
        own, first, second, both = blocks
        return jnp.stack([own, swap(first, "g1"), swap(second, "g2"), swap_both(both)])

    def share(unit):
        across = swap(unit, "s1")
        return [unit, swap(unit, "s2"), across, swap(across, "s2")]

    attn_unit = to_owners(columns("pack_attn", query_w, key_w, outer_gate_w, value_w))
    conv_unit = to_owners(columns("pack_conv", inner_gate_w, signal_w))
    out_width = channels + q_width
    out_unit = to_owners(
        call(
            pack_rows_kernel,
            [struct(out_conv_w.shape[1], out_width)] * 4,
            ids,
            out_conv_w,
            out_attn_w,
            specs=[SMEM, VMEM, VMEM],
            flops=1 << 20,
            name="pack_out",
        )
    )
    normed = call(
        norm_kernel,
        struct(k_blocks, rows, k_width),
        ids,
        tokens,
        other_tokens,
        norm_gain.reshape(1, -1),
        specs=[SMEM, VMEM, VMEM, VMEM],
        flops=1 << 22,
        name="norm",
    )
    across = swap(normed, "g1")
    normed = [normed, across, swap(normed, "g2"), swap(across, "g2")]
    normed = normed + [swap(value, "tp") for value in normed]

    attn_pieces, conv_pieces, out_pieces = share(attn_unit), share(conv_unit), share(out_unit)
    length = 8 * rows

    def project(name, pieces, tail_of, tail):
        width = pieces[0].shape[2]
        return call(
            functools.partial(project_kernel, tail_of),
            [struct(8, rows, width), struct(*tail)],
            ids,
            *normed,
            *pieces,
            specs=[SMEM] + [VMEM] * 12,
            flops=2 * length * k_blocks * k_width * width,
            scratch=[pltpu.VMEM((length, width), F32)],
            name=name,
        )

    def to_next(tail):
        return swap(tail, "s2"), lax.ppermute(tail[1:], ("s1", "s2"), [(1, 2)])

    attn_in, tail = project("project_attn", attn_pieces, kv_tail, (2, rows, 2 * HEAD))
    kv_halo = to_next(tail)
    conv_in, tail = project("project_conv", conv_pieces, conv_tail, (2, 16, 2 * channels))
    conv_halo = to_next(tail)
    part = lax.axis_index("g1") * 2 + lax.axis_index("g2")
    taps = lax.dynamic_index_in_dim(conv_taps.reshape(TAPS, 4, channels), part, 1, keepdims=False)
    act = call(
        functools.partial(mixer_kernel, (heads, channels)),
        struct(8, rows, out_width),
        ids,
        sink_logits,
        taps,
        attn_in,
        conv_in,
        *kv_halo,
        *conv_halo,
        specs=[SMEM, SMEM] + [VMEM] * 7,
        out_specs=pl.BlockSpec((1, rows, out_width), lambda i: (i, 0, 0)),
        grid=(8,),
        flops=length * 4 * rows * heads * HEAD * 2,
        name="mixer",
    )

    order = (((0, 0), (0, 1)), ((1, 0),), ((1, 1),))
    last = []
    for group in order:
        pieces = [out_pieces[a * 2 + b] for a, b in group]
        width = len(group) * 4 * out_conv_w.shape[1]
        sent, kept = call(
            functools.partial(project_out_kernel, len(group)),
            [struct(4, rows, width), struct(4, rows, width)],
            ids,
            act,
            *pieces,
            specs=[SMEM] + [VMEM] * (1 + len(group)),
            flops=2 * length * out_width * width,
            name="project_out",
        )
        got = swap(sent, "tp")
        second = swap((kept[2:].astype(F32) + got[2:].astype(F32)).astype(BF16), "g2")
        third = (kept[1].astype(F32) + got[1].astype(F32) + second[1].astype(F32)).astype(BF16)
        last += [kept, got, second, swap(third, "g1")]
    specs = []
    for n, value in enumerate(last):
        if n % 4 == 3:
            specs.append(VMEM)
        else:
            specs.append(pl.BlockSpec((1,) + value.shape[1:], lambda i: (0, 0, 0)))
    return call(
        functools.partial(assemble_kernel, order),
        struct(rows, k_blocks * k_width),
        ids,
        *last,
        specs=[SMEM] + specs,
        grid=(1,),
        flops=1 << 20,
        name="assemble",
    )


def from_behind(value, axis, steps):
    count = lax.axis_size(axis)
    initial, last = (max(0, -steps), min(count, count - steps))
    return lax.ppermute(value, axis, [(source, source + steps) for source in range(initial, last)])


def attention(queries, keys_ext, values_ext, sink_logits, offset):
    length = queries.shape[0]
    kv_local = keys_ext.shape[1] // HEAD
    group = QHEADS // KVHEADS
    heads_local = kv_local * group
    first = lax.axis_index("tp") * heads_local + 1
    slopes = jnp.exp2(
        -8.0 * (first + jnp.arange(heads_local, dtype=jnp.int32)).astype(F32) / QHEADS
    ).reshape(kv_local, group)
    sinks = sink_logits.reshape(kv_local, group)[:, :, None]
    qblock = queries.reshape(length, kv_local, group, HEAD)
    kblock = keys_ext.reshape(length + WINDOW, kv_local, HEAD)
    vblock = values_ext.reshape(length + WINDOW, kv_local, HEAD)
    scores = jnp.einsum("qhgd,shd->hgqs", qblock, kblock, preferred_element_type=F32) * HEAD ** (-0.5)
    qpos = offset + jnp.arange(length, dtype=jnp.int32)
    kpos = offset - WINDOW + jnp.arange(length + WINDOW, dtype=jnp.int32)
    dist = qpos[:, None] - kpos[None, :]
    valid = (dist >= 0) & (dist < WINDOW) & (kpos >= 0)[None, :]
    scores = scores - slopes[:, :, None, None] * dist.astype(F32)
    scores = jnp.where(valid, scores, -1e30)
    top = jnp.maximum(jnp.max(scores, axis=-1), sinks)
    expo = jnp.exp(scores - top[..., None])
    total = jnp.sum(expo, axis=-1) + jnp.exp(sinks - top)
    probs = (expo / total[..., None]).astype(BF16)
    out = jnp.einsum("hgqs,shd->qhgd", probs, vblock, preferred_element_type=F32)
    return out.reshape(length, heads_local * HEAD).astype(BF16)


def plain_body(
    tokens,
    norm_gain,
    outer_gate_w,
    inner_gate_w,
    signal_w,
    conv_taps,
    query_w,
    key_w,
    value_w,
    sink_logits,
    out_conv_w,
    out_attn_w,
):
    whole = lax.all_gather(tokens, "tp", axis=1, tiled=True)
    x32 = whole.astype(F32)
    normed = (x32 * lax.rsqrt(jnp.mean(x32 * x32, axis=-1, keepdims=True) + EPS) * norm_gain).astype(BF16)
    length = normed.shape[0]
    offset = lax.axis_index("sp") * length
    weights = (outer_gate_w, inner_gate_w, signal_w, query_w, key_w, value_w)
    whole_w = lax.all_gather(jnp.concatenate(weights, axis=1), "sp", axis=0, tiled=True)
    mixed = jnp.dot(normed, whole_w, preferred_element_type=F32).astype(BF16)
    ends, at = [], 0
    for w in weights[:-1]:
        at += w.shape[1]
        ends.append(at)
    outer, inner, signal, queries, keys, values = jnp.split(mixed, ends, axis=1)
    gated = (inner.astype(F32) * signal.astype(F32)).astype(BF16)
    before = from_behind(gated[length - TAPS + 1 :], "sp", 1)
    extended = jnp.concatenate([before, gated], axis=0).astype(F32)
    conv = sum(conv_taps[k] * extended[k : k + length] for k in range(TAPS))
    conv_out = (outer.astype(F32) * conv).astype(BF16)
    keys_before, values_before = from_behind((keys[length - WINDOW :], values[length - WINDOW :]), "sp", 1)
    keys_ext = jnp.concatenate([keys_before, keys], axis=0)
    values_ext = jnp.concatenate([values_before, values], axis=0)
    attn_out = attention(queries, keys_ext, values_ext, sink_logits, offset)
    conv_whole, attn_whole = (
        lax.all_gather(out_conv_w, "sp", axis=1, tiled=True),
        lax.all_gather(out_attn_w, "sp", axis=1, tiled=True),
    )
    result = jnp.dot(conv_out, conv_whole, preferred_element_type=F32)
    result = result + jnp.dot(attn_out, attn_whole, preferred_element_type=F32)
    return lax.psum_scatter(result.astype(BF16), "tp", scatter_dimension=0, tiled=True)


def splits(mesh, tokens, query_w):
    sp, tp = mesh.shape["sp"], mesh.shape["tp"]
    return (
        tp == 2
        and KVHEADS == 4 * tp
        and sp == 16
        and tokens.shape[0] == sp * tp * WINDOW
        and query_w.shape[0] % (sp // 2 * 128) == 0
        and query_w.shape[1] == QHEADS * HEAD
    )


def solution(mesh):
    def run(*args):
        fits = splits(mesh, args[0], args[6])
        if fits:
            names = ("s1", "g1", "s2", "g2")
            own = Mesh(mesh.devices.reshape(2, 2, 2, 2, 2), names + ("tp",))
        else:
            names, own = ("sp",), mesh
        wide = P(names, "tp")
        in_specs = (wide, P(), wide, wide, wide, P(None, "tp"), wide, wide, wide, P("tp"), P("tp", names), P("tp", names))
        return jax.shard_map(
            body if fits else plain_body,
            mesh=own,
            in_specs=in_specs,
            out_specs=P(names + ("tp",), None),
            check_vma=False,
        )(*args)

    return run
```
